512 devices in a mesh: fs: 64 (over z, y), tp: 8 (over x, core).
Axes of the slice: x: 4, y: 8, z: 8, core: 2. Of those that a mesh axis runs over, the one named last changes fastest.
Arguments:
- tokens: bfloat16 [49152, 2048], P('fs'), may hold values from -6 to 6
- norm_gain: float32 [2048], replicated, may hold values from 0.1 to 1.9
- up_weight: float32 [2048, 8192], P('fs', 'tp'), may hold values from -0.125 to 0.125
- up_scale: float32 [8192], P('tp'), may hold values from 0.5 to 2
- down_weight: float32 [8192, 2048], P('tp', 'fs'), may hold values from -0.1875 to 0.1875
- down_scale: float32 [1, 2048], replicated, may hold values from 0.5 to 2
Outputs:
- mixed: bfloat16 [49152, 2048], P('fs', 'tp')
The draws below stay inside these ranges and needn't reach their ends.
All inputs are finite; a program needn't handle non-finite values.
Results may differ from the reference program's by a relative error of at most 0.014.
Values may be sent and summed in bfloat16 or wider, within the bound.
A program may use at most 64 MiB of HBM per device.

```python
import math
import jax
import jax.numpy as jnp
from jax import lax

D = 2048
FF = 8192
TOKENS = 49152
N_FS = 64
N_TP = 8


def with_spikes(drawn, stream_key, source, target, shards_of, factor):
    def block_of(axis_at):
        return (jnp.arange(drawn.shape[axis_at]) // (drawn.shape[axis_at] // shards_of)).reshape((-1,) + (1,) * (drawn.ndim - 1 - axis_at))

    near = jax.random.permutation(stream_key, shards_of)[block_of(target)]
    far = (block_of(target) + shards_of // 2) % shards_of
    return jnp.where((block_of(source) == near) | (block_of(source) == far), factor * drawn, drawn)


def level_of(key, extent, cuts, low, high):
    level = 1.0
    for dim, shards_of in cuts:
        draws = jax.random.uniform(jax.random.fold_in(jax.random.fold_in(key, 6), dim), (shards_of,), jnp.float32, low / len(cuts), high / len(cuts))
        level = level * jnp.repeat(jnp.exp(draws), extent[dim] // shards_of).reshape((-1,) + (1,) * (len(extent) - 1 - dim))
    return level


def bell_draw(stream_key, extent, deviation, bound, shards=(), dtype=jnp.bfloat16):
    factor_of = level_of(stream_key, extent, shards, -0.22, 0.18) if shards else 1.0
    drawn = jax.random.normal(stream_key, extent, jnp.float32) * deviation * factor_of
    return jnp.minimum(jnp.maximum(drawn, -bound), bound).astype(dtype)


def gaussian_with(key, shape, spread, most, pieces, heavy, held_as=jnp.bfloat16):
    drawn = spread * jax.random.normal(key, shape, jnp.float32)
    if pieces:
        drawn = drawn * level_of(key, shape, pieces, -0.22, 0.18)
    return jnp.clip(with_spikes(drawn, jax.random.fold_in(key, 3), *heavy), -most, most).astype(held_as)


def setup_inputs(seed: int = 0) -> dict:
    arg_keys = jax.random.split(jax.random.key(seed), 7)
    tokens = bell_draw(arg_keys[0], (TOKENS, D), 1.0, 6.0, ((0, 64),))
    norm_gain = jnp.clip(1.0 + 0.18 * jax.random.normal(arg_keys[1], (D,), jnp.float32), 0.1, 1.9)
    up_weight = bell_draw(arg_keys[2], (D, FF), D ** -0.5, 0.125, ((0, 64), (1, 8)), jnp.float32)
    up_scale = jnp.clip(jnp.exp(math.log(2.0) - 1.3862944 * jax.random.uniform(arg_keys[3], (FF,), jnp.float32) ** level_of(arg_keys[3], (FF,), ((0, 8),), -0.2, 0.2)), 0.5, 2.0)
    down_weight = gaussian_with(arg_keys[4], (FF, D), FF ** -0.5, 0.1875, ((0, 8), (1, 64)), (0, 1, 64, 4.0), jnp.float32)
    down_scale = jnp.clip(jnp.exp(jax.random.uniform(arg_keys[5], (1, D), jnp.float32, math.log(0.5), math.log(2.0))), 0.5, 2.0)
    return dict(tokens=tokens, norm_gain=norm_gain, up_weight=up_weight, up_scale=up_scale, down_weight=down_weight, down_scale=down_scale)


def reference(tokens, norm_gain, up_weight, up_scale, down_weight, down_scale):
    up_cast = up_weight.astype(jnp.bfloat16)
    down_cast = down_weight.astype(jnp.bfloat16)
    block_ff = FF // N_TP
    groups = tokens.reshape(N_FS, TOKENS // N_FS, D)

    def one_group(rows):
        values = rows.astype(jnp.float32)
        normed = (values * lax.rsqrt(lax.optimization_barrier(jnp.mean(values * values, axis=-1, keepdims=True)) + 1e-06) * norm_gain).astype(jnp.bfloat16)
        pre = jnp.dot(normed, up_cast, preferred_element_type=jnp.float32) * up_scale
        hidden = jnp.square(jnp.maximum(pre, 0.0)).astype(jnp.bfloat16)
        total = jnp.zeros((rows.shape[0], D), jnp.float32)
        for block in range(N_TP):
            lower = block * block_ff
            partial_value = jnp.dot(hidden[:, lower:lower + block_ff], down_cast[lower:lower + block_ff, :], preferred_element_type=jnp.float32) * down_scale
            total = total + partial_value.astype(jnp.bfloat16).astype(jnp.float32)
        return total.astype(jnp.bfloat16)
    return lax.map(one_group, groups).reshape(TOKENS, D)
```

```python
import functools
import heapq

import jax
import jax.numpy as jnp
from jax import lax
from jax.experimental import pallas as pl
from jax.experimental.pallas import tpu as pltpu
from jax.sharding import PartitionSpec as P

MESH = pl.DeviceIdType.MESH
R = 8
COLS = (0, 1, -1, 2, -2, 3, -3, 4)
ROWS = 16
WIRE, HOP, DEPTH = 0.703, 2.0, 3


def limits(t):
    return (4, 3) if t == 0 else (3, 4)


def col_rank(d):
    return COLS.index(4 if d == -4 else d)


def build_messages():
    msgs = {}
    for t in (0, 1):
        plus, minus = limits(t)
        offs = range(-minus, plus + 1)
        for h in (0, 1):
            first, second = ("y", "z") if h == 0 else ("z", "y")
            for d in offs:
                if d == 0:
                    continue
                s = 1 if d > 0 else -1
                msgs[(t, h, 1, d, 0)] = ((first, -s), None if abs(d) == 1 else (t, h, 1, d - s, 0))
            for f in offs:
                for d in offs:
                    if d == 0:
                        continue
                    s = 1 if d > 0 else -1
                    if abs(d) == 1:
                        dep = None if f == 0 else (t, h, 1, f, 0)
                    else:
                        dep = (t, h, 2, f, d - s)
                    msgs[(t, h, 2, f, d)] = ((second, -s), dep)
    return msgs


def offset_yz(k):
    _, h, _, f, s = k
    return (f, s) if h == 0 else (s, f)


def priority(k):
    t, h, ph, f, s = k
    if ph == 1:
        return (0 if t == 0 else 0.5, abs(f), 0)
    if t == 0:
        return (1, col_rank(f) + abs(s) if h == 0 else col_rank(s) + abs(f) * 0.1, 0)
    return (2, col_rank(f if h == 0 else s), -abs(s))


def simulate(msgs):
    children, heaps = {}, {}
    for k, (link, dep) in msgs.items():
        heaps.setdefault(link, [])
        if dep is None:
            heapq.heappush(heaps[link], (priority(k), k))
        else:
            children.setdefault(dep, []).append(k)
    queued = {l: 0 for l in heaps}
    until = {l: 0.0 for l in heaps}
    issued, arrival, events, count = [], {}, [], 0

    def fill(link, now):
        nonlocal count
        while queued[link] < DEPTH and heaps[link]:
            _, k = heapq.heappop(heaps[link])
            end = max(now, until[link]) + WIRE
            until[link] = end
            queued[link] += 1
            issued.append((now, k))
            count += 1
            heapq.heappush(events, (end, count, 0, link))
            count += 1
            heapq.heappush(events, (end + HOP, count, 1, k))

    for l in heaps:
        fill(l, 0.0)
    while events:
        now, _, kind, x = heapq.heappop(events)
        if kind == 0:
            queued[x] -= 1
            fill(x, now)
        else:
            arrival[x] = now
            for c in children.get(x, ()):
                link = msgs[c][0]
                heapq.heappush(heaps[link], (priority(c), c))
                fill(link, now)
    return issued, arrival


def plan():
    msgs = build_messages()
    issued, arrival = simulate(msgs)
    steps, waited = [], set()

    def wait_for(keys):
        for k in sorted(keys, key=lambda m: (arrival[m], m)):
            if k not in waited:
                waited.add(k)
                steps.append(("wait", k))

    up_keys = [k for k in msgs if k[0] == 0]
    col_keys = []
    for d in COLS:
        here = [k for k in msgs if k[0] == 1 and offset_yz(k)[0] in ((d, -d) if d == 4 else (d,))]
        col_keys.append(here)
    now, at = 0.0, 0
    tasks = [("norm", i) for i in range(6)]
    ready = {t: 1.5 for t in tasks}
    cost = {"norm": 0.35, "up": 0.5, "D": 0.9, "E": 0.25, "F": 0.15, "G": 0.1}
    up_ready = max(arrival[k] for k in up_keys)
    for i in range(8):
        tasks.append(("up", i))
        ready[("up", i)] = up_ready
    for i in range(8):
        tasks.append(("D", i))
        ready[("D", i)] = max(arrival[k] for k in col_keys[i])
    after = {"D": ("E", 2.0), "E": ("F", 3.0), "F": ("G", 3.5)}
    rank = {"G": 0, "F": 1, "E": 2, "norm": 3, "up": 4, "D": 5}
    while at < len(issued) or tasks:
        if at < len(issued) and issued[at][0] <= now + 0.05:
            k = issued[at][1]
            dep = msgs[k][1]
            if dep is not None:
                wait_for([dep])
            steps.append(("send", k))
            at += 1
            now += 0.01
            continue
        usable = [t for t in tasks if ready[t] <= now]
        firsts = {}
        for t in tasks:
            firsts.setdefault(t[0], t)
        usable = [t for t in usable if firsts[t[0]] == t]
        if any(t[0] == "norm" for t in tasks):
            usable = [t for t in usable if t[0] == "norm"]
        elif any(t[0] == "up" for t in tasks):
            usable = [t for t in usable if t[0] == "up"]
        if usable:
            t = min(usable, key=lambda u: rank[u[0]])
            tasks.remove(t)
            if t[0] == "up":
                wait_for(up_keys)
            if t[0] == "D":
                wait_for(col_keys[t[1]])
            steps.append(t)
            now += cost[t[0]]
            if t[0] in after:
                nxt, lag = after[t[0]]
                tasks.append((nxt, t[1]))
                ready[(nxt, t[1])] = now + lag
            continue
        times = [ready[t] for t in tasks if ready[t] > now]
        if at < len(issued):
            times.append(issued[at][0])
        now = max(now + 0.01, min(times)) if times else now + 0.01
    wait_for(msgs)
    return msgs, steps


def kernel(
    msgs, steps, index,
    tok_hbm, gain_ref, upw_ref, upsc_ref, dnw_ref, dnsc_ref, out_ref,
    tok, up_buf, dn_buf, hid, psend, precv, pown, sbuf, r1, fbuf, gbuf, out_t,
    tok_sem, w_send, w_recv, d_send, d_recv, s_send, s_recv, f_send, f_recv,
):
    fs, tp = lax.axis_index("fs"), lax.axis_index("tp")
    z, y = lax.div(fs, R), lax.rem(fs, R)
    x, c = lax.div(tp, 2), lax.rem(tp, 2)

    def near(axis, g):
        if axis == "y":
            return (z * R + lax.rem(y + (g + R), R), tp)
        if axis == "z":
            return (lax.rem(z + (g + R), R) * R + y, tp)
        return (fs, lax.rem(x + (g + 4), 4) * 2 + c)

    links = {(a, g): near(a, g) for a in "yz" for g in (1, -1)}
    right, left = near("x", 1), near("x", -1)
    partner = (fs, x * 2 + 1 - c)

    barrier = pltpu.get_barrier_semaphore()
    peers = list(links.values()) + [right, left, partner]
    for peer in peers:
        pl.semaphore_signal(barrier, inc=1, device_id=peer, device_id_type=MESH)

    tok_copy = pltpu.make_async_copy(tok_hbm, tok, tok_sem)
    tok_copy.start()

    bufs = (up_buf, dn_buf)
    ys = {d: lax.rem(y + (d + R), R) for d in range(-4, 5)}
    zs = {d: lax.rem(z + (d + R), R) for d in range(-4, 5)}

    def shard_row(dy, dz):
        return zs[dz] * 256 + ys[dy] * 32

    mine = pl.multiple_of(shard_row(0, 0), 32)
    up_buf[pl.ds(mine, 32), :] = upw_ref[...].astype(jnp.bfloat16)
    dn_buf[pl.ds(mine, 32), :] = dnw_ref[...].astype(jnp.bfloat16)

    pl.semaphore_wait(barrier, len(peers))

    def copy_of(k, sending):
        axis, g = msgs[k][0]
        dy, dz = offset_yz(k)
        if sending:
            dy, dz = (dy + g, dz) if axis == "y" else (dy, dz + g)
        row = pl.multiple_of(shard_row(dy, dz) + k[1] * ROWS, ROWS)
        ref = bufs[k[0]].at[pl.ds(row, ROWS), :]
        return pltpu.make_async_remote_copy(
            src_ref=ref, dst_ref=ref,
            send_sem=w_send.at[k[0] * 2 + k[1]], recv_sem=w_recv.at[index[k]],
            device_id=links[(axis, g)], device_id_type=MESH,
        )

    def norm(i):
        if i == 0:
            tok_copy.wait()
        rows = pl.ds(i * 128, 128)
        v = tok[rows, :].astype(jnp.float32)
        scale = lax.rsqrt(jnp.mean(v * v, axis=-1, keepdims=True) + 1e-6)
        tok[rows, :] = (v * scale * gain_ref[...]).astype(jnp.bfloat16)

    def up(i):
        n, half = i // 2, i % 2
        cols = pl.ds(n * 256, 256)
        rows = pl.ds(half * 384, 384)
        pre = jnp.dot(tok[rows, :], up_buf[:, cols], preferred_element_type=jnp.float32)
        pre = jnp.maximum(pre * upsc_ref[:, cols], 0.0)
        hid[cols, rows] = (pre * pre).T.astype(jnp.bfloat16)

    def partial(i, parity):
        row = ys[COLS[i]] * 32 + parity * 256
        lhs = jnp.concatenate(
            [dn_buf[pl.ds(pl.multiple_of(row + k * 512, 32), 32), :] for k in range(4)], axis=0
        )
        return jnp.dot(lhs, hid[...], preferred_element_type=jnp.float32)

    def pair_copy(i):
        return pltpu.make_async_remote_copy(
            src_ref=psend.at[i], dst_ref=precv.at[i], send_sem=d_send, recv_sem=d_recv.at[i],
            device_id=partner, device_id_type=MESH,
        )

    def relay_copy(i, side):
        return pltpu.make_async_remote_copy(
            src_ref=sbuf.at[i, side], dst_ref=r1.at[i, side], send_sem=s_send, recv_sem=s_recv.at[i, side],
            device_id=(right, left)[side], device_id_type=MESH,
        )

    def final_copy(i, side):
        return pltpu.make_async_remote_copy(
            src_ref=fbuf.at[i, side], dst_ref=gbuf.at[i, side], send_sem=f_send, recv_sem=f_recv.at[i, side],
            device_id=(right, left)[side], device_id_type=MESH,
        )

    def step_d(i):
        psend[i] = partial(i, 1 - c).reshape(4, 32, 768).astype(jnp.bfloat16)
        pown[i] = partial(i, c).reshape(4, 32, 768)
        pair_copy(i).start()

    def step_e(i):
        pair_copy(i).wait_recv()
        far = lax.rem(x + 2, 4)
        for q in range(1, 5):
            k = lax.rem(far + q, 4)
            if q == 1:
                total = pown[i, far] + precv[i, far].astype(jnp.float32)
                sbuf[i, 0] = total[:16].astype(jnp.bfloat16)
                sbuf[i, 1] = total[16:].astype(jnp.bfloat16)
            if q < 4:
                pown[i, k] = pown[i, k] + precv[i, k].astype(jnp.float32)
        relay_copy(i, 0).start()
        relay_copy(i, 1).start()

    def step_f(i):
        for side in (0, 1):
            relay_copy(i, side).wait_recv()
            k = lax.rem(x + (1, 3)[side], 4)
            own = pown[i, k]
            extra = r1[i, side].astype(jnp.float32)
            top, bottom = own[:16], own[16:]
            if side == 0:
                top = top + extra
            else:
                bottom = bottom + extra
            fbuf[i, side, :16, :] = top.astype(jnp.bfloat16)
            fbuf[i, side, 16:, :] = bottom.astype(jnp.bfloat16)
            final_copy(i, side).start()

    def step_g(i):
        final_copy(i, 0).wait_recv()
        final_copy(i, 1).wait_recv()
        total = pown[i, x] + gbuf[i, 0].astype(jnp.float32) + gbuf[i, 1].astype(jnp.float32)
        out_t[pl.ds(pl.multiple_of(ys[COLS[i]] * 32, 32), 32), :] = total

    run = {"norm": norm, "up": up, "D": step_d, "E": step_e, "F": step_f, "G": step_g}
    for name, arg in steps:
        if name == "wait":
            copy_of(arg, False).wait_recv()
        elif name == "send":
            copy_of(arg, True).start()
        else:
            run[name](arg)

    scale = dnsc_ref[:, pl.ds(pl.multiple_of(tp * 256, 256), 256)]
    out_ref[...] = (out_t[...].T * scale).astype(jnp.bfloat16)

    def sent(ref, sem):
        pltpu.make_async_copy(ref, ref, sem).wait()

    for t in (0, 1):
        for h in (0, 1):
            sent(bufs[t].at[pl.ds(0, 63 * ROWS), :], w_send.at[t * 2 + h])
    sent(psend, d_send)
    sent(sbuf, s_send)
    sent(fbuf, f_send)


def on_device(tokens, norm_gain, up_weight, up_scale, down_weight, down_scale):
    msgs, steps = plan()
    index = {k: i for i, k in enumerate(msgs)}
    vmem = pl.BlockSpec(memory_space=pltpu.VMEM)
    bf16, f32 = jnp.bfloat16, jnp.float32
    dma = pltpu.SemaphoreType.DMA
    return pl.pallas_call(
        functools.partial(kernel, msgs, steps, index),
        out_shape=jax.ShapeDtypeStruct((768, 256), bf16),
        in_specs=[pl.BlockSpec(memory_space=pl.ANY)] + [vmem] * 5,
        out_specs=vmem,
        scratch_shapes=[
            pltpu.VMEM((768, 2048), bf16),
            pltpu.VMEM((2048, 1024), bf16),
            pltpu.VMEM((2048, 1024), bf16),
            pltpu.VMEM((1024, 768), bf16),
            pltpu.VMEM((8, 4, 32, 768), bf16),
            pltpu.VMEM((8, 4, 32, 768), bf16),
            pltpu.VMEM((8, 4, 32, 768), f32),
            pltpu.VMEM((8, 2, 16, 768), bf16),
            pltpu.VMEM((8, 2, 16, 768), bf16),
            pltpu.VMEM((8, 2, 32, 768), bf16),
            pltpu.VMEM((8, 2, 32, 768), bf16),
            pltpu.VMEM((256, 768), f32),
            dma, dma((4,)), dma((len(msgs),)), dma, dma((8,)), dma, dma((8, 2)), dma, dma((8, 2)),
        ],
        compiler_params=pltpu.CompilerParams(collective_id=0, has_side_effects=True),
    )(
        tokens, norm_gain.reshape(1, -1), up_weight, up_scale.reshape(1, -1), down_weight.T,
        down_scale,
    )


def solution(mesh):
    in_specs = (P("fs", None), P(), P("fs", "tp"), P("tp"), P("tp", "fs"), P())
    return jax.shard_map(
        on_device, mesh=mesh, in_specs=in_specs, out_specs=P("fs", "tp"), check_vma=False
    )
```

```python
import functools
import heapq

import jax
import jax.numpy as jnp
from jax import lax
from jax.experimental import pallas as pl
from jax.experimental.pallas import tpu as pltpu
from jax.sharding import PartitionSpec as P

MESH = pl.DeviceIdType.MESH
R = 8
COLS = (0, 1, -1, 2, -2, 3, -3, 4)
ROWS = 16
DIRECT = (6, 7)
RELAYED = (0, 1, 2, 3, 4, 5)
WIRE, HOP, PAIR, DEPTH = 0.703, 2.6, 1.6, 2
COST = {"norm": 0.22, "U": 0.17, "V": 0.45, "D": 0.57, "E": 0.05, "F": 0.03, "G": 0.02}
BASE, FIRST, NEXT = (1, 16), (0, 1), 1
BLOCK, STEP, LATE, SECOND = (0.2, 1), (1, 1.5), (2, -1), (1, 0.8)


def limits(t):
    return (4, 3) if t == 0 else (3, 4)


def axes(t, h):
    return ("z", "y") if t == h else ("y", "z")


def block_of(k):
    _, h, _, f, s = k
    d = f if h == 0 else s
    return COLS.index(4 if d == -4 else d)


def offset_yz(k):
    t, h, _, f, s = k
    return (f, s) if axes(t, h)[0] == "y" else (s, f)


def build_messages():
    msgs = {}
    for t in (0, 1):
        plus, minus = limits(t)
        offs = range(-minus, plus + 1)
        for h in (0, 1):
            first, second = axes(t, h)
            for d in offs:
                if d == 0:
                    continue
                s = 1 if d > 0 else -1
                msgs[(t, h, 1, d, 0)] = ((first, -s), None if abs(d) == 1 else (t, h, 1, d - s, 0))
            for f in offs:
                for d in offs:
                    if d == 0:
                        continue
                    s = 1 if d > 0 else -1
                    if abs(d) == 1:
                        dep = None if f == 0 else (t, h, 1, f, 0)
                    else:
                        dep = (t, h, 2, f, d - s)
                    msgs[(t, h, 2, f, d)] = ((second, -s), dep)
    return msgs


def priority(k):
    t, h, ph, f, s = k
    if ph == 1:
        return FIRST[t] + NEXT * abs(f)
    if h == 0:
        return BASE[t] + BLOCK[t] * block_of(k) + STEP[t] * abs(s)
    return BASE[t] + SECOND[t] * block_of(k) + 0.01 * abs(f) + LATE[t]


def plan():
    msgs = build_messages()
    children, heaps = {}, {}
    for k, (link, dep) in msgs.items():
        heaps.setdefault(link, [])
        if dep is None:
            heapq.heappush(heaps[link], (priority(k), k))
        else:
            children.setdefault(dep, []).append(k)
    ends = {link: [] for link in heaps}
    wires = [0.0, 0.0]
    arrival, pending, steps, waited, done, ready = {}, [], [], set(), {}, {}
    tasks = [("norm", i) for i in range(6)] + [("U", i) for i in range(32)] + [("D", i) for i in range(8)]
    rank = {"G": 0, "F": 0, "E": 0, "norm": 2, "U": 3, "D": 4}
    blocks = {(t, i): [k for k in msgs if k[0] == t and block_of(k) == i] for t in (0, 1) for i in range(8)}
    now, ups = 0.0, 0

    def wait_for(keys):
        for k in sorted(keys, key=lambda m: (arrival[m], m)):
            if k not in waited:
                waited.add(k)
                steps.append(("wait", k))

    def ready_at(task):
        kind, i = task
        if task not in ready:
            if kind == "norm":
                ready[task] = 0.3
            else:
                need = blocks[(0, i // 4) if kind == "U" else (1, i)]
                before = ("norm", 5) if kind == "U" else ("U", 31)
                if (before in done if kind == "U" else ups == 32) and all(k in arrival for k in need):
                    ready[task] = max(arrival[k] for k in need)
        return ready.get(task, 1e9)

    def on_wires(us):
        for q in (0, 1):
            wires[q] = max(wires[q], now) + us
        return max(wires)

    while True:
        while pending and pending[0][0] <= now:
            for c in children.get(heapq.heappop(pending)[1], ()):
                heapq.heappush(heaps[msgs[c][0]], (priority(c), c))
        best = None
        for link, heap in heaps.items():
            ends[link] = [e for e in ends[link] if e > now]
            if heap and len(ends[link]) < DEPTH:
                key = (len(ends[link]), heap[0][0])
                if best is None or key < best[0]:
                    best = (key, link)
        if best is not None:
            link = best[1]
            k = heapq.heappop(heaps[link])[1]
            if msgs[k][1] is not None:
                wait_for([msgs[k][1]])
            steps.append(("send", k))
            ends[link].append(max([now] + ends[link]) + WIRE)
            arrival[k] = ends[link][-1] + HOP
            heapq.heappush(pending, (arrival[k], k))
            now += 0.012
            continue
        usable = [
            (rank[t[0]], ready_at(t) if t[0] in "UD" else t[1], t) for t in tasks if ready_at(t) <= now
        ]
        if usable:
            task = min(usable)[2]
            tasks.remove(task)
            kind, i = task
            if kind == "U":
                wait_for(blocks[0, i // 4])
                ups += 1
            if kind == "D":
                wait_for(blocks[1, i])
            steps.append(task)
            now += COST["V" if kind == "U" and ups > 28 else kind]
            done[task] = now
            if kind == "D":
                tasks.append(("E", i))
                ready["E", i] = now + PAIR
            if kind == "E" and i in DIRECT:
                tasks.append(("G", i))
                ready["G", i] = on_wires(1.6) + HOP + 0.8
            elif kind == "E":
                tasks.append(("F", i))
                ready["F", i] = on_wires(0.52) + HOP
            if kind == "F":
                tasks.append(("G", i))
                ready["G", i] = on_wires(1.05) + HOP
            continue
        later = [p[0] for p in pending[:1]]
        later += [ends[link][0] for link in heaps if heaps[link] and ends[link]]
        later += [ready_at(t) for t in tasks if now < ready_at(t) < 1e9]
        if not later:
            break
        now = max(now + 1e-6, min(later))
    wait_for(msgs)
    return msgs, steps


def kernel(
    msgs, steps, index,
    tok_hbm, gain_ref, upw_ref, upsc_ref, dnw_ref, dnsc_ref, out_ref,
    tok, up_buf, dn_buf, acc, hid, psend, precv, pown, sbuf, r1, fbuf, gbuf, ebuf, hbuf, out_t,
    tok_sem, w_send, w_recv, d_send, d_recv, s_send, s_recv, f_send, f_recv, e_send, e_recv,
):
    fs, tp = lax.axis_index("fs"), lax.axis_index("tp")
    z, y = lax.div(fs, R), lax.rem(fs, R)
    x, c = lax.div(tp, 2), lax.rem(tp, 2)

    def near(axis, g):
        if axis == "y":
            return (z * R + lax.rem(y + (g + R), R), tp)
        if axis == "z":
            return (lax.rem(z + (g + R), R) * R + y, tp)
        return (fs, lax.rem(x + (g + 4), 4) * 2 + c)

    links = {(a, g): near(a, g) for a in "yz" for g in (1, -1)}
    right, left, far = near("x", 1), near("x", -1), near("x", 2)
    partner = (fs, x * 2 + 1 - c)

    barrier = pltpu.get_barrier_semaphore()
    peers = list(links.values()) + [right, left, far, partner]
    for peer in peers:
        pl.semaphore_signal(barrier, inc=1, device_id=peer, device_id_type=MESH)

    tok_copy = pltpu.make_async_copy(tok_hbm, tok, tok_sem)
    tok_copy.start()

    bufs = (up_buf, dn_buf)
    ys = {d: lax.rem(y + (d + R), R) for d in range(-4, 5)}
    zs = {d: lax.rem(z + (d + R), R) for d in range(-4, 5)}

    def shard_row(dy, dz):
        return zs[dz] * 256 + ys[dy] * 32

    mine = pl.multiple_of(shard_row(0, 0), 32)
    up_buf[pl.ds(mine, 32), :] = upw_ref[...].astype(jnp.bfloat16)
    dn_buf[pl.ds(mine, 32), :] = dnw_ref[...].astype(jnp.bfloat16)

    pl.semaphore_wait(barrier, len(peers))

    def copy_of(k, sending):
        axis, g = msgs[k][0]
        dy, dz = offset_yz(k)
        if sending:
            dy, dz = (dy + g, dz) if axis == "y" else (dy, dz + g)
        row = pl.multiple_of(shard_row(dy, dz) + k[1] * ROWS, ROWS)
        ref = bufs[k[0]].at[pl.ds(row, ROWS), :]
        return pltpu.make_async_remote_copy(
            src_ref=ref, dst_ref=ref,
            send_sem=w_send.at[k[0] * 2 + k[1]], recv_sem=w_recv.at[index[k]],
            device_id=links[(axis, g)], device_id_type=MESH,
        )

    def norm(i):
        if i == 0:
            tok_copy.wait()
        rows = pl.ds(i * 128, 128)
        v = tok[rows, :].astype(jnp.float32)
        scale = lax.rsqrt(jnp.mean(v * v, axis=-1, keepdims=True) + 1e-6)
        tok[rows, :] = (v * scale * gain_ref[...]).astype(jnp.bfloat16)

    seen = [0] * 4

    def up(j):
        i, n = j // 4, j % 4
        cols = pl.ds(n * 256, 256)
        depth = pl.ds(pl.multiple_of(zs[COLS[i]] * 256, 256), 256)
        pre = jnp.dot(tok[:, depth], up_buf[depth, cols], preferred_element_type=jnp.float32)
        if seen[n] > 0:
            pre = acc[:, cols] + pre
        if seen[n] < 7:
            acc[:, cols] = pre
        else:
            pre = jnp.maximum(pre * upsc_ref[:, cols], 0.0)
            hid[cols, :] = (pre * pre).T.astype(jnp.bfloat16)
        seen[n] += 1

    def partial(i, parity):
        row = ys[COLS[i]] * 32 + parity * 256
        lhs = jnp.concatenate(
            [dn_buf[pl.ds(pl.multiple_of(row + k * 512, 32), 32), :] for k in range(4)], axis=0
        )
        return jnp.dot(lhs, hid[...], preferred_element_type=jnp.float32)

    def pair_copy(i):
        return pltpu.make_async_remote_copy(
            src_ref=psend.at[i], dst_ref=precv.at[i], send_sem=d_send, recv_sem=d_recv.at[i],
            device_id=partner, device_id_type=MESH,
        )

    def relay_copy(i, side):
        return pltpu.make_async_remote_copy(
            src_ref=sbuf.at[RELAYED.index(i), side], dst_ref=r1.at[RELAYED.index(i), side],
            send_sem=s_send, recv_sem=s_recv.at[RELAYED.index(i), side],
            device_id=(right, left)[side], device_id_type=MESH,
        )

    def final_copy(i, side):
        return pltpu.make_async_remote_copy(
            src_ref=fbuf.at[RELAYED.index(i), side], dst_ref=gbuf.at[RELAYED.index(i), side],
            send_sem=f_send, recv_sem=f_recv.at[RELAYED.index(i), side],
            device_id=(right, left)[side], device_id_type=MESH,
        )

    def step_d(i):
        psend[i] = partial(i, 1 - c).reshape(4, 32, 768).astype(jnp.bfloat16)
        pown[i] = partial(i, c).reshape(4, 32, 768)
        pair_copy(i).start()

    def direct_copy(i, way):
        return pltpu.make_async_remote_copy(
            src_ref=ebuf.at[DIRECT.index(i), way], dst_ref=hbuf.at[DIRECT.index(i), way],
            send_sem=e_send, recv_sem=e_recv.at[DIRECT.index(i), way],
            device_id=(far, right, left)[way], device_id_type=MESH,
        )

    def summed(i, k):
        return pown[i, k] + precv[i, k].astype(jnp.float32)

    def step_e(i):
        pair_copy(i).wait_recv()
        k_far, k_right, k_left = lax.rem(x + 2, 4), lax.rem(x + 1, 4), lax.rem(x + 3, 4)
        if i in DIRECT:
            for way, k in enumerate((k_far, k_right, k_left)):
                ebuf[DIRECT.index(i), way] = summed(i, k).astype(jnp.bfloat16)
            for way in (0, 1, 2):
                direct_copy(i, way).start()
            pown[i, x] = summed(i, x)
        else:
            r = RELAYED.index(i)
            total = summed(i, k_far).astype(jnp.bfloat16)
            sbuf[r, 0] = total[:16]
            sbuf[r, 1] = total[16:]
            for k in (k_right, k_left):
                pown[i, k] = summed(i, k)
            relay_copy(i, 0).start()
            relay_copy(i, 1).start()
            pown[i, x] = summed(i, x)

    def step_f(i):
        for side in (0, 1):
            relay_copy(i, side).wait_recv()
            k = lax.rem(x + (1, 3)[side], 4)
            own = pown[i, k]
            extra = r1[RELAYED.index(i), side].astype(jnp.float32)
            top, bottom = own[:16], own[16:]
            if side == 0:
                top = top + extra
            else:
                bottom = bottom + extra
            fbuf[RELAYED.index(i), side, :16, :] = top.astype(jnp.bfloat16)
            fbuf[RELAYED.index(i), side, 16:, :] = bottom.astype(jnp.bfloat16)
            final_copy(i, side).start()

    def step_g(i):
        total = pown[i, x]
        if i in DIRECT:
            for way in (0, 1, 2):
                direct_copy(i, way).wait_recv()
                total = total + hbuf[DIRECT.index(i), way].astype(jnp.float32)
        else:
            for side in (0, 1):
                final_copy(i, side).wait_recv()
                total = total + gbuf[RELAYED.index(i), side].astype(jnp.float32)
        out_t[pl.ds(pl.multiple_of(ys[COLS[i]] * 32, 32), 32), :] = total

    run = {"norm": norm, "U": up, "D": step_d, "E": step_e, "F": step_f, "G": step_g}
    for name, arg in steps:
        if name == "wait":
            copy_of(arg, False).wait_recv()
        elif name == "send":
            copy_of(arg, True).start()
        else:
            run[name](arg)

    scale = dnsc_ref[:, pl.ds(pl.multiple_of(tp * 256, 256), 256)]
    out_ref[...] = (out_t[...].T * scale).astype(jnp.bfloat16)

    def sent(ref, sem):
        pltpu.make_async_copy(ref, ref, sem).wait()

    for t in (0, 1):
        for h in (0, 1):
            sent(bufs[t].at[pl.ds(0, 63 * ROWS), :], w_send.at[t * 2 + h])
    sent(psend, d_send)
    sent(sbuf, s_send)
    sent(fbuf, f_send)
    sent(ebuf, e_send)


def on_device(tokens, norm_gain, up_weight, up_scale, down_weight, down_scale):
    msgs, steps = plan()
    index = {k: i for i, k in enumerate(msgs)}
    vmem = pl.BlockSpec(memory_space=pltpu.VMEM)
    bf16, f32 = jnp.bfloat16, jnp.float32
    dma = pltpu.SemaphoreType.DMA
    relayed, direct = len(RELAYED), len(DIRECT)
    return pl.pallas_call(
        functools.partial(kernel, msgs, steps, index),
        out_shape=jax.ShapeDtypeStruct((768, 256), bf16),
        in_specs=[pl.BlockSpec(memory_space=pl.ANY)] + [vmem] * 5,
        out_specs=vmem,
        scratch_shapes=[
            pltpu.VMEM((768, 2048), bf16),
            pltpu.VMEM((2048, 1024), bf16),
            pltpu.VMEM((2048, 1024), bf16),
            pltpu.VMEM((768, 1024), f32),
            pltpu.VMEM((1024, 768), bf16),
            pltpu.VMEM((8, 4, 32, 768), bf16),
            pltpu.VMEM((8, 4, 32, 768), bf16),
            pltpu.VMEM((8, 4, 32, 768), f32),
            pltpu.VMEM((relayed, 2, 16, 768), bf16),
            pltpu.VMEM((relayed, 2, 16, 768), bf16),
            pltpu.VMEM((relayed, 2, 32, 768), bf16),
            pltpu.VMEM((relayed, 2, 32, 768), bf16),
            pltpu.VMEM((direct, 3, 32, 768), bf16),
            pltpu.VMEM((direct, 3, 32, 768), bf16),
            pltpu.VMEM((256, 768), f32),
            dma, dma((4,)), dma((len(msgs),)), dma, dma((8,)),
            dma, dma((relayed, 2)), dma, dma((relayed, 2)), dma, dma((direct, 3)),
        ],
        compiler_params=pltpu.CompilerParams(collective_id=0, has_side_effects=True),
    )(
        tokens, norm_gain.reshape(1, -1), up_weight, up_scale.reshape(1, -1), down_weight.T,
        down_scale,
    )


def solution(mesh):
    in_specs = (P("fs", None), P(), P("fs", "tp"), P("tp"), P("tp", "fs"), P())
    return jax.shard_map(
        on_device, mesh=mesh, in_specs=in_specs, out_specs=P("fs", "tp"), check_vma=False
    )
```

```python
import functools
import heapq

import jax
import jax.numpy as jnp
from jax import lax
from jax.experimental import pallas as pl
from jax.experimental.pallas import tpu as pltpu
from jax.sharding import PartitionSpec as P

MESH = pl.DeviceIdType.MESH
R = 8
COLS = (0, 1, -1, 2, -2, 3, -3, 4)
ROWS = 16
WIRE, HOP, PAIR, DEPTH = 0.703, 2.6, 1.8, 2
COST = {"norm": 0.22, "U": 0.23, "V": 0.43, "D": 0.57, "E": 0.05, "F": 0.03, "G": 0.02}
BASE, FIRST, NEXT = (1, 20), (0, 9), 0.1
BLOCK, STEP, LATE, SECOND = (0, 1), (2, 3), (-2, -2), (0.8, 1.3)


def limits(t):
    return (4, 3) if t == 0 else (3, 4)


def axes(t, h):
    return ("z", "y") if t == h else ("y", "z")


def block_of(k):
    _, h, _, f, s = k
    d = f if h == 0 else s
    return COLS.index(4 if d == -4 else d)


def offset_yz(k):
    t, h, _, f, s = k
    return (f, s) if axes(t, h)[0] == "y" else (s, f)


def build_messages():
    msgs = {}
    for t in (0, 1):
        plus, minus = limits(t)
        offs = range(-minus, plus + 1)
        for h in (0, 1):
            first, second = axes(t, h)
            for d in offs:
                if d == 0:
                    continue
                s = 1 if d > 0 else -1
                msgs[(t, h, 1, d, 0)] = ((first, -s), None if abs(d) == 1 else (t, h, 1, d - s, 0))
            for f in offs:
                for d in offs:
                    if d == 0:
                        continue
                    s = 1 if d > 0 else -1
                    if abs(d) == 1:
                        dep = None if f == 0 else (t, h, 1, f, 0)
                    else:
                        dep = (t, h, 2, f, d - s)
                    msgs[(t, h, 2, f, d)] = ((second, -s), dep)
    return msgs


def priority(k):
    t, h, ph, f, s = k
    if ph == 1:
        return FIRST[t] + NEXT * abs(f)
    if h == 0:
        return BASE[t] + BLOCK[t] * block_of(k) + STEP[t] * abs(s)
    return BASE[t] + SECOND[t] * block_of(k) + 0.01 * abs(f) + LATE[t]


def plan():
    msgs = build_messages()
    children, heaps = {}, {}
    for k, (link, dep) in msgs.items():
        heaps.setdefault(link, [])
        if dep is None:
            heapq.heappush(heaps[link], (priority(k), k))
        else:
            children.setdefault(dep, []).append(k)
    ends = {link: [] for link in heaps}
    wires = [0.0, 0.0]
    arrival, pending, steps, waited, done, ready = {}, [], [], set(), {}, {}
    tasks = [("norm", i) for i in range(6)] + [("U", i) for i in range(32)] + [("D", i) for i in range(8)]
    rank = {"G": 0, "F": 0, "E": 0, "norm": 2, "U": 3, "D": 4}
    blocks = {(t, i): [k for k in msgs if k[0] == t and block_of(k) == i] for t in (0, 1) for i in range(8)}
    now, ups = 0.0, 0

    def wait_for(keys):
        for k in sorted(keys, key=lambda m: (arrival[m], m)):
            if k not in waited:
                waited.add(k)
                steps.append(("wait", k))

    def ready_at(task):
        kind, i = task
        if task not in ready:
            if kind == "norm":
                ready[task] = 0.3
            else:
                need = blocks[(0, i // 4) if kind == "U" else (1, i)]
                before = ("norm", 5) if kind == "U" else ("U", 31)
                if (before in done if kind == "U" else ups == 32) and all(k in arrival for k in need):
                    ready[task] = max(arrival[k] for k in need)
        return ready.get(task, 1e9)

    def on_wires(us):
        for q in (0, 1):
            wires[q] = max(wires[q], now) + us
        return max(wires)

    while True:
        while pending and pending[0][0] <= now:
            for c in children.get(heapq.heappop(pending)[1], ()):
                heapq.heappush(heaps[msgs[c][0]], (priority(c), c))
        best = None
        for link, heap in heaps.items():
            ends[link] = [e for e in ends[link] if e > now]
            if heap and len(ends[link]) < DEPTH:
                key = (len(ends[link]), heap[0][0])
                if best is None or key < best[0]:
                    best = (key, link)
        if best is not None:
            link = best[1]
            k = heapq.heappop(heaps[link])[1]
            if msgs[k][1] is not None:
                wait_for([msgs[k][1]])
            steps.append(("send", k))
            ends[link].append(max([now] + ends[link]) + WIRE)
            arrival[k] = ends[link][-1] + HOP
            heapq.heappush(pending, (arrival[k], k))
            now += 0.012
            continue
        usable = [
            (rank[t[0]], ready_at(t) if t[0] in "UD" else t[1], t) for t in tasks if ready_at(t) <= now
        ]
        if usable:
            task = min(usable)[2]
            tasks.remove(task)
            kind, i = task
            if kind == "U":
                wait_for(blocks[0, i // 4])
                ups += 1
            if kind == "D":
                wait_for(blocks[1, i])
            steps.append(task)
            now += COST["V" if kind == "U" and ups > 28 else kind]
            done[task] = now
            if kind == "D":
                tasks.append(("E", i))
                ready["E", i] = now + PAIR
            if kind == "E":
                tasks.append(("F", i))
                ready["F", i] = on_wires(0.52) + HOP
            if kind == "F":
                tasks.append(("G", i))
                ready["G", i] = on_wires(1.05) + HOP
            continue
        later = [p[0] for p in pending[:1]]
        later += [ends[link][0] for link in heaps if heaps[link] and ends[link]]
        later += [ready_at(t) for t in tasks if now < ready_at(t) < 1e9]
        if not later:
            break
        now = max(now + 1e-6, min(later))
    wait_for(msgs)
    return msgs, steps


def kernel(
    msgs, steps, index,
    tok_hbm, gain_hbm, upw_hbm, upsc_hbm, dnw_hbm, dnsc_hbm, out_ref,
    tok, gain_ref, upw_ref, upsc_ref, dnw_ref, dnsc_ref,
    up_buf, dn_buf, acc, hid, psend, precv, pown, sbuf, r1, fbuf, gbuf, out_t,
    in_sem, w_send, w_recv, d_send, d_recv, s_send, s_recv, f_send, f_recv,
):
    fs, tp = lax.axis_index("fs"), lax.axis_index("tp")
    z, y = lax.div(fs, R), lax.rem(fs, R)
    x, c = lax.div(tp, 2), lax.rem(tp, 2)

    def near(axis, g):
        if axis == "y":
            return (z * R + lax.rem(y + (g + R), R), tp)
        if axis == "z":
            return (lax.rem(z + (g + R), R) * R + y, tp)
        return (fs, lax.rem(x + (g + 4), 4) * 2 + c)

    links = {(a, g): near(a, g) for a in "yz" for g in (1, -1)}
    right, left = near("x", 1), near("x", -1)
    partner = (fs, x * 2 + 1 - c)

    barrier = pltpu.get_barrier_semaphore()
    peers = list(links.values()) + [right, left, partner]
    for peer in peers:
        pl.semaphore_signal(barrier, inc=1, device_id=peer, device_id_type=MESH)

    pairs = (
        (upw_hbm, upw_ref), (dnw_hbm, dnw_ref), (tok_hbm, tok),
        (gain_hbm, gain_ref), (upsc_hbm, upsc_ref), (dnsc_hbm, dnsc_ref),
    )
    loads = [pltpu.make_async_copy(a, b, in_sem.at[n]) for n, (a, b) in enumerate(pairs)]
    for load in loads:
        load.start()

    bufs = (up_buf, dn_buf)
    ys = {d: lax.rem(y + (d + R), R) for d in range(-4, 5)}
    zs = {d: lax.rem(z + (d + R), R) for d in range(-4, 5)}

    def shard_row(dy, dz):
        return zs[dz] * 256 + ys[dy] * 32

    mine = pl.multiple_of(shard_row(0, 0), 32)
    loads[0].wait()
    up_buf[pl.ds(mine, 32), :] = upw_ref[...].astype(jnp.bfloat16)
    loads[1].wait()
    dn_buf[pl.ds(mine, 32), :] = dnw_ref[...].astype(jnp.bfloat16)

    pl.semaphore_wait(barrier, len(peers))

    def copy_of(k, sending):
        axis, g = msgs[k][0]
        dy, dz = offset_yz(k)
        if sending:
            dy, dz = (dy + g, dz) if axis == "y" else (dy, dz + g)
        row = pl.multiple_of(shard_row(dy, dz) + k[1] * ROWS, ROWS)
        ref = bufs[k[0]].at[pl.ds(row, ROWS), :]
        return pltpu.make_async_remote_copy(
            src_ref=ref, dst_ref=ref,
            send_sem=w_send.at[k[0] * 2 + k[1]], recv_sem=w_recv.at[index[k]],
            device_id=links[(axis, g)], device_id_type=MESH,
        )

    def norm(i):
        if i == 0:
            for load in loads[2:]:
                load.wait()
        rows = pl.ds(i * 128, 128)
        v = tok[rows, :].astype(jnp.float32)
        scale = lax.rsqrt(jnp.mean(v * v, axis=-1, keepdims=True) + 1e-6)
        tok[rows, :] = (v * scale * gain_ref[...]).astype(jnp.bfloat16)

    seen = [0] * 4

    def up(j):
        i, n = j // 4, j % 4
        cols = pl.ds(n * 256, 256)
        depth = pl.ds(pl.multiple_of(zs[COLS[i]] * 256, 256), 256)
        pre = jnp.dot(tok[:, depth], up_buf[depth, cols], preferred_element_type=jnp.float32)
        if seen[n] > 0:
            pre = acc[:, cols] + pre
        if seen[n] < 7:
            acc[:, cols] = pre
        else:
            pre = jnp.maximum(pre * upsc_ref[:, cols], 0.0)
            hid[cols, :] = (pre * pre).T.astype(jnp.bfloat16)
        seen[n] += 1

    def partial(i, parity):
        row = ys[COLS[i]] * 32 + parity * 256
        lhs = jnp.concatenate(
            [dn_buf[pl.ds(pl.multiple_of(row + k * 512, 32), 32), :] for k in range(4)], axis=0
        )
        return jnp.dot(lhs, hid[...], preferred_element_type=jnp.float32)

    def pair_copy(i):
        return pltpu.make_async_remote_copy(
            src_ref=psend.at[i], dst_ref=precv.at[i], send_sem=d_send, recv_sem=d_recv.at[i],
            device_id=partner, device_id_type=MESH,
        )

    def relay_copy(i, side):
        return pltpu.make_async_remote_copy(
            src_ref=sbuf.at[i, side], dst_ref=r1.at[i, side],
            send_sem=s_send, recv_sem=s_recv.at[i, side],
            device_id=(right, left)[side], device_id_type=MESH,
        )

    def final_copy(i, side):
        return pltpu.make_async_remote_copy(
            src_ref=fbuf.at[i, side], dst_ref=gbuf.at[i, side],
            send_sem=f_send, recv_sem=f_recv.at[i, side],
            device_id=(right, left)[side], device_id_type=MESH,
        )

    def step_d(i):
        psend[i] = partial(i, 1 - c).reshape(4, 32, 768).astype(jnp.bfloat16)
        pown[i] = partial(i, c).reshape(4, 32, 768)
        pair_copy(i).start()

    def summed(i, k):
        return pown[i, k] + precv[i, k].astype(jnp.float32)

    def step_e(i):
        pair_copy(i).wait_recv()
        k_far, k_right, k_left = lax.rem(x + 2, 4), lax.rem(x + 1, 4), lax.rem(x + 3, 4)
        total = summed(i, k_far).astype(jnp.bfloat16)
        sbuf[i, 0] = total[:16]
        sbuf[i, 1] = total[16:]
        for k in (k_right, k_left):
            pown[i, k] = summed(i, k)
        relay_copy(i, 0).start()
        relay_copy(i, 1).start()
        pown[i, x] = summed(i, x)

    def step_f(i):
        for side in (0, 1):
            relay_copy(i, side).wait_recv()
            k = lax.rem(x + (1, 3)[side], 4)
            own = pown[i, k]
            extra = r1[i, side].astype(jnp.float32)
            top, bottom = own[:16], own[16:]
            if side == 0:
                top = top + extra
            else:
                bottom = bottom + extra
            fbuf[i, side, :16, :] = top.astype(jnp.bfloat16)
            fbuf[i, side, 16:, :] = bottom.astype(jnp.bfloat16)
            final_copy(i, side).start()

    def step_g(i):
        total = pown[i, x]
        for side in (0, 1):
            final_copy(i, side).wait_recv()
            total = total + gbuf[i, side].astype(jnp.float32)
        out_t[pl.ds(pl.multiple_of(ys[COLS[i]] * 32, 32), 32), :] = total

    run = {"norm": norm, "U": up, "D": step_d, "E": step_e, "F": step_f, "G": step_g}
    for name, arg in steps:
        if name == "wait":
            copy_of(arg, False).wait_recv()
        elif name == "send":
            copy_of(arg, True).start()
        else:
            run[name](arg)

    scale = dnsc_ref[:, pl.ds(pl.multiple_of(tp * 256, 256), 256)]
    out_ref[...] = (out_t[...].T * scale).astype(jnp.bfloat16)

    def sent(ref, sem):
        pltpu.make_async_copy(ref, ref, sem).wait()

    for t in (0, 1):
        for h in (0, 1):
            sent(bufs[t].at[pl.ds(0, 63 * ROWS), :], w_send.at[t * 2 + h])
    sent(psend, d_send)
    sent(sbuf, s_send)
    sent(fbuf, f_send)


def scoped_kernel(msgs, steps, index, *refs):
    dma = pltpu.SemaphoreType.DMA
    pl.run_scoped(
        functools.partial(kernel, msgs, steps, index, *refs),
        dma((6,)), dma((4,)), dma((len(msgs),)), dma, dma((8,)),
        dma, dma((8, 2)), dma, dma((8, 2)),
    )


def on_device(tokens, norm_gain, up_weight, up_scale, down_weight, down_scale):
    msgs, steps = plan()
    index = {k: i for i, k in enumerate(msgs)}
    bf16, f32 = jnp.bfloat16, jnp.float32
    return pl.pallas_call(
        functools.partial(scoped_kernel, msgs, steps, index),
        out_shape=pltpu.VMEM((768, 256), bf16),
        in_specs=[pl.BlockSpec(memory_space=pl.ANY)] * 6,
        out_specs=pl.BlockSpec(memory_space=pltpu.VMEM),
        scratch_shapes=[
            pltpu.VMEM((768, 2048), bf16),
            pltpu.VMEM((1, 2048), f32),
            pltpu.VMEM((32, 1024), f32),
            pltpu.VMEM((1, 1024), f32),
            pltpu.VMEM((32, 1024), f32),
            pltpu.VMEM((1, 2048), f32),
            pltpu.VMEM((2048, 1024), bf16),
            pltpu.VMEM((2048, 1024), bf16),
            pltpu.VMEM((768, 1024), f32),
            pltpu.VMEM((1024, 768), bf16),
            pltpu.VMEM((8, 4, 32, 768), bf16),
            pltpu.VMEM((8, 4, 32, 768), bf16),
            pltpu.VMEM((8, 4, 32, 768), f32),
            pltpu.VMEM((8, 2, 16, 768), bf16),
            pltpu.VMEM((8, 2, 16, 768), bf16),
            pltpu.VMEM((8, 2, 32, 768), bf16),
            pltpu.VMEM((8, 2, 32, 768), bf16),
            pltpu.VMEM((256, 768), f32),
        ],
        compiler_params=pltpu.CompilerParams(collective_id=0, has_side_effects=True),
    )(
        tokens, norm_gain.reshape(1, -1), up_weight, up_scale.reshape(1, -1), down_weight.T,
        down_scale,
    )


def solution(mesh):
    in_specs = (P("fs", None), P(), P("fs", "tp"), P("tp"), P("tp", "fs"), P())
    return jax.shard_map(
        on_device, mesh=mesh, in_specs=in_specs, out_specs=P("fs", "tp"), check_vma=False
    )
```

```python
import functools
import heapq

import jax
import jax.numpy as jnp
from jax import lax
from jax.experimental import pallas as pl
from jax.experimental.pallas import tpu as pltpu
from jax.sharding import PartitionSpec as P

MESH = pl.DeviceIdType.MESH
R = 8
COLS = (0, 1, -1, 2, -2, 3, -3, 4)
ROWS = 16
WIRE, HOP, WAY, PAIR, DEPTH = 0.703, 2.8, 3.1, 1.8, 2
STEP = 16.31
COST = {"norm": 0.22, "U": 0.28, "V": 0.44, "D": 0.45, "E": 0.05, "F": 0.03, "G": 0.02}

DUE = (
    (
        (-1.3, -38.8, 6.0, -11.0, -24.6, 19.5, -16.2, -18.6),
        (-15.4, 23.0, 56.1, 14.3, 17.4, -10.9, 5.5, 7.4),
    ),
    (
        (61.4, 19.4, 63.9, 44.6, 47.9, 26.6, 68.4, 62.4),
        (23.2, 34.6, 92.2, 95.6, 155.2, 56.9, 54.7, 59.9),
    ),
)


def axes(t, h):
    return ("z", "y") if t == h else ("y", "z")


def offsets(t, f=0):
    return range(-3, 5) if (t + f) % 2 == 0 else range(-4, 4)


def block_of(k):
    _, h, _, f, s = k
    d = f if h == 0 else s
    return COLS.index(4 if d == -4 else d)


def offset_yz(k):
    t, h, _, f, s = k
    return (f, s) if axes(t, h)[0] == "y" else (s, f)


def build_messages():
    msgs = {}
    for t in (0, 1):
        for h in (0, 1):
            first, second = axes(t, h)
            for d in offsets(t):
                s = 1 if d > 0 else -1
                if d:
                    msgs[(t, h, 1, d, 0)] = ((first, -s), None if abs(d) == 1 else (t, h, 1, d - s, 0))
            for f in offsets(t):
                for d in offsets(t, f):
                    s = 1 if d > 0 else -1
                    if abs(d) == 1:
                        dep = None if f == 0 else (t, h, 1, f, 0)
                    else:
                        dep = (t, h, 2, f, d - s)
                    if d:
                        msgs[(t, h, 2, f, d)] = ((second, -s), dep)
    return msgs


def due_times(msgs):
    due = {}
    for k in sorted(msgs, key=lambda m: -abs(m[3]) - abs(m[4])):
        due[k] = min(due.get(k, 1e9), DUE[k[0]][k[1]][block_of(k)])
        dep = msgs[k][1]
        if dep is not None:
            due[dep] = min(due.get(dep, 1e9), due[k] - STEP)
    return due


def plan(log=None):
    msgs = build_messages()
    children, heaps = {}, {}
    due = due_times(msgs)
    for k, (link, dep) in msgs.items():
        heaps.setdefault(link, [])
        if dep is None:
            heapq.heappush(heaps[link], (due[k], k))
        else:
            children.setdefault(dep, []).append(k)
    ends = {link: [] for link in heaps}
    wires = [0.0, 0.0]
    arrival, pending, steps, waited, ready = {}, [], [], set(), {}
    tasks = [("norm", i) for i in range(6)] + [("U", i) for i in range(32)] + [("D", i) for i in range(16)]
    rank = {"G": 1, "F": 0, "E": 0, "norm": 2, "U": 3, "D": 4}
    blocks = {(0, i): [k for k in msgs if k[0] == 0 and block_of(k) == i] for i in range(8)}
    blocks.update({(1, i): [k for k in msgs if k[:2] == (1, i % 2) and block_of(k) == i // 2] for i in range(16)})
    now, ups, norms = 0.0, 0, 0

    def wait_for(keys):
        for k in sorted(keys, key=lambda m: (arrival[m], m)):
            if k not in waited:
                waited.add(k)
                steps.append(("wait", k))

    def ready_at(task):
        kind, i = task
        if task not in ready:
            if kind == "norm":
                ready[task] = 0.3
            else:
                need = blocks[(0, i // 4) if kind == "U" else (1, i)]
                if (norms == 6 if kind == "U" else ups == 32) and all(k in arrival for k in need):
                    ready[task] = max(arrival[k] for k in need)
        return ready.get(task, 1e9)

    def on_wires(us):
        for q in (0, 1):
            wires[q] = max(wires[q], now) + us
        return max(wires)

    while True:
        while pending and pending[0][0] <= now:
            k = heapq.heappop(pending)[1]
            for c in children.get(k, ()):
                heapq.heappush(heaps[msgs[c][0]], (due[c], c))
        best = None
        for link, heap in heaps.items():
            ends[link] = [e for e in ends[link] if e > now]
            if heap and len(ends[link]) < DEPTH:
                key = (len(ends[link]), heap[0][0])
                if best is None or key < best[0]:
                    best = (key, link)
        if best is not None:
            link = best[1]
            k = heapq.heappop(heaps[link])[1]
            if msgs[k][1] is not None:
                wait_for([msgs[k][1]])
            steps.append(("send", k))
            ends[link].append(max([now] + ends[link]) + WIRE)
            arrival[k] = ends[link][-1] + HOP
            heapq.heappush(pending, (arrival[k], k))
            now += 0.012
            continue
        usable = [
            (rank[t[0]], ready_at(t) if t[0] in "UD" else t[1], t) for t in tasks if ready_at(t) <= now
        ]
        if usable:
            task = min(usable)[2]
            tasks.remove(task)
            kind, i = task
            norms += kind == "norm"
            if kind == "U":
                wait_for(blocks[0, i // 4])
                ups += 1
            if kind == "D":
                wait_for(blocks[1, i])
            steps.append(task)
            if log is not None:
                log.append((now, task))
            now += COST["V" if kind == "U" and ups > 28 else kind]
            if kind == "D":
                tasks.append(("E", i))
                ready["E", i] = now + PAIR
            if kind == "E":
                tasks.append(("F", i))
                ready["F", i] = on_wires(0.26) + WAY
            if kind == "F":
                tasks.append(("G", i))
                ready["G", i] = on_wires(0.52) + WAY + 0.8
            continue
        later = [p[0] for p in pending[:1]]
        later += [ends[link][0] for link in heaps if heaps[link] and ends[link]]
        later += [ready_at(t) for t in tasks if now < ready_at(t) < 1e9]
        if not later:
            break
        now = max(now + 1e-6, min(later))
    wait_for(msgs)
    if log is not None:
        log.append((now, max(arrival.values()), max(v for k, v in arrival.items() if k[0] == 0)))
    return msgs, steps


def kernel(
    msgs, steps, index,
    tok_hbm, gain_hbm, upw_hbm, upsc_hbm, dnw_hbm, dnsc_hbm, out_ref,
    tok, gain_ref, upw_ref, upsc_ref, dnw_ref, dnsc_ref,
    up_buf, dn_buf, acc, hid, psend, precv, pown, sbuf, r1, fbuf, gbuf, out_t,
    in_sem, w_send, w_recv, d_send, d_recv, s_send, s_recv, f_send, f_recv,
):
    fs, tp = lax.axis_index("fs"), lax.axis_index("tp")
    z, y = lax.div(fs, R), lax.rem(fs, R)
    x, c = lax.div(tp, 2), lax.rem(tp, 2)

    def near(axis, g):
        if axis == "y":
            return (z * R + lax.rem(y + (g + R), R), tp)
        if axis == "z":
            return (lax.rem(z + (g + R), R) * R + y, tp)
        return (fs, lax.rem(x + (g + 4), 4) * 2 + c)

    links = {(a, g): near(a, g) for a in "yz" for g in (1, -1)}
    right, left = near("x", 1), near("x", -1)
    partner = (fs, x * 2 + 1 - c)

    barrier = pltpu.get_barrier_semaphore()
    peers = list(links.values()) + [right, left, partner]
    for peer in peers:
        pl.semaphore_signal(barrier, inc=1, device_id=peer, device_id_type=MESH)

    pairs = (
        (upw_hbm, upw_ref), (dnw_hbm, dnw_ref), (tok_hbm, tok),
        (gain_hbm, gain_ref), (upsc_hbm, upsc_ref), (dnsc_hbm, dnsc_ref),
    )
    loads = [pltpu.make_async_copy(a, b, in_sem.at[n]) for n, (a, b) in enumerate(pairs)]
    for load in loads:
        load.start()

    bufs = (up_buf, dn_buf)
    ys = {d: lax.rem(y + (d + R), R) for d in range(-4, 5)}
    zs = {d: lax.rem(z + (d + R), R) for d in range(-4, 5)}

    def shard_row(dy, dz):
        return zs[dz] * 256 + ys[dy] * 32

    mine = pl.multiple_of(shard_row(0, 0), 32)
    loads[0].wait()
    up_buf[pl.ds(mine, 32), :] = upw_ref[...].astype(jnp.bfloat16)
    loads[1].wait()
    dn_buf[pl.ds(mine, 32), :] = dnw_ref[...].astype(jnp.bfloat16)

    pl.semaphore_wait(barrier, len(peers))

    def copy_of(k, sending):
        axis, g = msgs[k][0]
        dy, dz = offset_yz(k)
        if sending:
            dy, dz = (dy + g, dz) if axis == "y" else (dy, dz + g)
        row = pl.multiple_of(shard_row(dy, dz) + k[1] * ROWS, ROWS)
        ref = bufs[k[0]].at[pl.ds(row, ROWS), :]
        return pltpu.make_async_remote_copy(
            src_ref=ref, dst_ref=ref,
            send_sem=w_send.at[k[0] * 2 + k[1]], recv_sem=w_recv.at[index[k]],
            device_id=links[(axis, g)], device_id_type=MESH,
        )

    def norm(i):
        if i == 0:
            for load in loads[2:]:
                load.wait()
        rows = pl.ds(i * 128, 128)
        v = tok[rows, :].astype(jnp.float32)
        scale = lax.rsqrt(jnp.mean(v * v, axis=-1, keepdims=True) + 1e-6)
        tok[rows, :] = (v * scale * gain_ref[...]).astype(jnp.bfloat16)

    seen = [0] * 4

    def up(j):
        i, n = j // 4, j % 4
        cols = pl.ds(n * 256, 256)
        depth = pl.ds(pl.multiple_of(zs[COLS[i]] * 256, 256), 256)
        pre = jnp.dot(tok[:, depth], up_buf[depth, cols], preferred_element_type=jnp.float32)
        if seen[n] > 0:
            pre = acc[:, cols] + pre
        if seen[n] < 7:
            acc[:, cols] = pre
        else:
            pre = jnp.maximum(pre * upsc_ref[:, cols], 0.0)
            hid[cols, :] = (pre * pre).T.astype(jnp.bfloat16)
        seen[n] += 1

    def pair_copy(i):
        return pltpu.make_async_remote_copy(
            src_ref=psend.at[i], dst_ref=precv.at[i], send_sem=d_send, recv_sem=d_recv.at[i],
            device_id=partner, device_id_type=MESH,
        )

    def relay_copy(i, side):
        return pltpu.make_async_remote_copy(
            src_ref=sbuf.at[i, side], dst_ref=r1.at[i, side], send_sem=s_send, recv_sem=s_recv.at[i, side],
            device_id=(right, left)[side], device_id_type=MESH,
        )

    def final_copy(i, side):
        return pltpu.make_async_remote_copy(
            src_ref=fbuf.at[i, side], dst_ref=gbuf.at[i, side], send_sem=f_send, recv_sem=f_recv.at[i, side],
            device_id=(right, left)[side], device_id_type=MESH,
        )

    def row_in_block(i):
        return ys[COLS[i // 2]] * 32 + (i % 2) * ROWS

    def step_d(i):
        rows = [row_in_block(i) + parity * 256 + k * 512 for parity in (1 - c, c) for k in range(4)]
        lhs = jnp.concatenate([dn_buf[pl.ds(pl.multiple_of(r, ROWS), ROWS), :] for r in rows], axis=0)
        part = jnp.dot(lhs, hid[...], preferred_element_type=jnp.float32)
        psend[i] = part[:64].reshape(4, ROWS, 768).astype(jnp.bfloat16)
        pown[i] = part[64:].reshape(4, ROWS, 768)
        pair_copy(i).start()

    def summed(i, k):
        return pown[i, k] + precv[i, k].astype(jnp.float32)

    def step_e(i):
        pair_copy(i).wait_recv()
        k_far, k_right, k_left = lax.rem(x + 2, 4), lax.rem(x + 1, 4), lax.rem(x + 3, 4)
        total = summed(i, k_far).astype(jnp.bfloat16)
        sbuf[i, 0] = total[:, :384]
        sbuf[i, 1] = total[:, 384:]
        for k in (k_right, k_left):
            pown[i, k] = summed(i, k)
        relay_copy(i, 0).start()
        relay_copy(i, 1).start()
        pown[i, x] = summed(i, x)

    def step_f(i):
        for side in (0, 1):
            relay_copy(i, side).wait_recv()
            own = pown[i, lax.rem(x + (1, 3)[side], 4)]
            extra = r1[i, side].astype(jnp.float32)
            head, tail = own[:, :384], own[:, 384:]
            if side == 0:
                head = head + extra
            else:
                tail = tail + extra
            fbuf[i, side, :, :384] = head.astype(jnp.bfloat16)
            fbuf[i, side, :, 384:] = tail.astype(jnp.bfloat16)
            final_copy(i, side).start()

    def step_g(i):
        total = pown[i, x]
        for side in (0, 1):
            final_copy(i, side).wait_recv()
            total = total + gbuf[i, side].astype(jnp.float32)
        out_t[pl.ds(pl.multiple_of(row_in_block(i), ROWS), ROWS), :] = total

    run = {"norm": norm, "U": up, "D": step_d, "E": step_e, "F": step_f, "G": step_g}
    for name, arg in steps:
        if name == "wait":
            copy_of(arg, False).wait_recv()
        elif name == "send":
            copy_of(arg, True).start()
        else:
            run[name](arg)

    scale = dnsc_ref[:, pl.ds(pl.multiple_of(tp * 256, 256), 256)]
    out_ref[...] = (out_t[...].T * scale).astype(jnp.bfloat16)

    def sent(ref, sem):
        pltpu.make_async_copy(ref, ref, sem).wait()

    for t in (0, 1):
        for h in (0, 1):
            sent(bufs[t].at[pl.ds(0, 63 * ROWS), :], w_send.at[t * 2 + h])
    sent(psend, d_send)
    sent(sbuf, s_send)
    sent(fbuf, f_send)


def scoped_kernel(msgs, steps, index, *refs):
    dma = pltpu.SemaphoreType.DMA
    pl.run_scoped(
        functools.partial(kernel, msgs, steps, index, *refs),
        dma((6,)), dma((4,)), dma((len(msgs),)), dma, dma((16,)),
        dma, dma((16, 2)), dma, dma((16, 2)),
    )


def on_device(tokens, norm_gain, up_weight, up_scale, down_weight, down_scale):
    msgs, steps = plan()
    index = {k: i for i, k in enumerate(msgs)}
    bf16, f32 = jnp.bfloat16, jnp.float32
    return pl.pallas_call(
        functools.partial(scoped_kernel, msgs, steps, index),
        out_shape=pltpu.VMEM((768, 256), bf16),
        in_specs=[pl.BlockSpec(memory_space=pl.ANY)] * 6,
        out_specs=pl.BlockSpec(memory_space=pltpu.VMEM),
        scratch_shapes=[
            pltpu.VMEM((768, 2048), bf16),
            pltpu.VMEM((1, 2048), f32),
            pltpu.VMEM((32, 1024), f32),
            pltpu.VMEM((1, 1024), f32),
            pltpu.VMEM((32, 1024), f32),
            pltpu.VMEM((1, 2048), f32),
            pltpu.VMEM((2048, 1024), bf16),
            pltpu.VMEM((2048, 1024), bf16),
            pltpu.VMEM((768, 1024), f32),
            pltpu.VMEM((1024, 768), bf16),
            pltpu.VMEM((16, 4, 16, 768), bf16),
            pltpu.VMEM((16, 4, 16, 768), bf16),
            pltpu.VMEM((16, 4, 16, 768), f32),
            pltpu.VMEM((16, 2, 16, 384), bf16),
            pltpu.VMEM((16, 2, 16, 384), bf16),
            pltpu.VMEM((16, 2, 16, 768), bf16),
            pltpu.VMEM((16, 2, 16, 768), bf16),
            pltpu.VMEM((256, 768), f32),
        ],
        compiler_params=pltpu.CompilerParams(collective_id=0, has_side_effects=True),
    )(
        tokens, norm_gain.reshape(1, -1), up_weight, up_scale.reshape(1, -1), down_weight.T,
        down_scale,
    )


def solution(mesh):
    in_specs = (P("fs", None), P(), P("fs", "tp"), P("tp"), P("tp", "fs"), P())
    return jax.shard_map(
        on_device, mesh=mesh, in_specs=in_specs, out_specs=P("fs", "tp"), check_vma=False
    )
```

```python
import functools
import heapq

import jax
import jax.numpy as jnp
from jax import lax
from jax.experimental import pallas as pl
from jax.experimental.pallas import tpu as pltpu
from jax.sharding import PartitionSpec as P

MESH = pl.DeviceIdType.MESH
R = 8
COLS = (0, 1, -1, 2, -2, 3, -3, 4)
ROWS = 16
WIRE, HOP, WAY, PAIR, DEPTH = 0.703, 2.8, 3.1, 1.8, 2
STEP = 18.94
COST = {"norm": 0.22, "U": 0.28, "V": 0.44, "D": 0.45, "E": 0.05, "F": 0.03, "G": 0.02, "L": 0.5, "M": 0.06}
LAST = 4

DUE = (
    (
        (4.1, -34.3, 16.5, -24.1, -49.3, -7.6, -41.5, -31.4),
        (-30.9, 12.5, 39.1, 34.0, 16.3, 4.0, 3.6, -15.7),
    ),
    (
        (64.3, 22.9, 71.7, 33.2, 46.6, 25.8, 72.8, 48.8),
        (36.3, 48.7, 88.5, 92.2, 145.0, 61.6, 55.4, 66.4),
    ),
)


def axes(t, h):
    return ("z", "y") if t == h else ("y", "z")


def offsets(t, f=0):
    return range(-3, 5) if (t + f) % 2 == 0 else range(-4, 4)


def block_of(k):
    _, h, _, f, s = k
    d = f if h == 0 else s
    return COLS.index(4 if d == -4 else d)


def offset_yz(k):
    t, h, _, f, s = k
    return (f, s) if axes(t, h)[0] == "y" else (s, f)


def build_messages():
    msgs = {}
    for t in (0, 1):
        for h in (0, 1):
            first, second = axes(t, h)
            for d in offsets(t):
                s = 1 if d > 0 else -1
                if d:
                    msgs[(t, h, 1, d, 0)] = ((first, -s), None if abs(d) == 1 else (t, h, 1, d - s, 0))
            for f in offsets(t):
                for d in offsets(t, f):
                    s = 1 if d > 0 else -1
                    if abs(d) == 1:
                        dep = None if f == 0 else (t, h, 1, f, 0)
                    else:
                        dep = (t, h, 2, f, d - s)
                    if d:
                        msgs[(t, h, 2, f, d)] = ((second, -s), dep)
    return msgs


def due_times(msgs):
    due = {}
    for k in sorted(msgs, key=lambda m: -abs(m[3]) - abs(m[4])):
        due[k] = min(due.get(k, 1e9), DUE[k[0]][k[1]][block_of(k)])
        dep = msgs[k][1]
        if dep is not None:
            due[dep] = min(due.get(dep, 1e9), due[k] - STEP)
    return due


def plan(log=None):
    msgs = build_messages()
    children, heaps = {}, {}
    due = due_times(msgs)
    for k, (link, dep) in msgs.items():
        heaps.setdefault(link, [])
        if dep is None:
            heapq.heappush(heaps[link], (due[k], k))
        else:
            children.setdefault(dep, []).append(k)
    ends = {link: [] for link in heaps}
    wires = [0.0, 0.0]
    arrival, pending, steps, waited, ready = {}, [], [], set(), {}
    tasks = [("norm", i) for i in range(6)] + [("U", i) for i in range(32)] + [("D", i) for i in range(16)]
    rank = {"G": 1, "M": 0, "F": 0, "E": 0, "norm": 2, "U": 3, "D": 4}
    blocks = {(0, i): [k for k in msgs if k[0] == 0 and block_of(k) == i] for i in range(8)}
    blocks.update({(1, i): [k for k in msgs if k[:2] == (1, i % 2) and block_of(k) == i // 2] for i in range(16)})
    now, ups, norms = 0.0, 0, 0

    def wait_for(keys):
        for k in sorted(keys, key=lambda m: (arrival[m], m)):
            if k not in waited:
                waited.add(k)
                steps.append(("wait", k))

    def ready_at(task):
        kind, i = task
        if task not in ready:
            if kind == "norm":
                ready[task] = 0.3
            else:
                need = blocks[(0, i // 4) if kind == "U" else (1, i)]
                if (norms == 6 if kind == "U" else ups == 32) and all(k in arrival for k in need):
                    ready[task] = max(arrival[k] for k in need)
        return ready.get(task, 1e9)

    def on_wires(us):
        for q in (0, 1):
            wires[q] = max(wires[q], now) + us
        return max(wires)

    while True:
        while pending and pending[0][0] <= now:
            k = heapq.heappop(pending)[1]
            for c in children.get(k, ()):
                heapq.heappush(heaps[msgs[c][0]], (due[c], c))
        best = None
        for link, heap in heaps.items():
            ends[link] = [e for e in ends[link] if e > now]
            if heap and len(ends[link]) < DEPTH:
                key = (len(ends[link]), heap[0][0])
                if best is None or key < best[0]:
                    best = (key, link)
        if best is not None:
            link = best[1]
            k = heapq.heappop(heaps[link])[1]
            if msgs[k][1] is not None:
                wait_for([msgs[k][1]])
            steps.append(("send", k))
            ends[link].append(max([now] + ends[link]) + WIRE)
            arrival[k] = ends[link][-1] + HOP
            heapq.heappush(pending, (arrival[k], k))
            now += 0.012
            continue
        usable = [
            (rank[t[0]], ready_at(t) if t[0] in "UD" else t[1], t) for t in tasks if ready_at(t) <= now
        ]
        if usable:
            task = min(usable)[2]
            tasks.remove(task)
            kind, i = task
            norms += kind == "norm"
            if kind == "U":
                wait_for(blocks[0, i // 4])
                ups += 1
            if kind == "D":
                wait_for(blocks[1, i])
            if kind == "D" and sum(t[0] == "D" for t in tasks) < LAST:
                kind, task = "L", ("L", i)
            steps.append(task)
            if log is not None:
                log.append((now, task))
            now += COST["V" if kind == "U" and ups > 28 else kind]
            if kind == "D":
                tasks.append(("E", i))
                ready["E", i] = now + PAIR
            if kind == "E":
                tasks.append(("F", i))
                ready["F", i] = on_wires(0.26) + WAY
            if kind == "L":
                tasks.append(("M", i))
                ready["M", i] = max(now + PAIR, on_wires(0.52) + WAY)
            if kind in "FM":
                tasks.append(("G", i))
                ready["G", i] = on_wires(0.52) + WAY + 0.8
            continue
        later = [p[0] for p in pending[:1]]
        later += [ends[link][0] for link in heaps if heaps[link] and ends[link]]
        later += [ready_at(t) for t in tasks if now < ready_at(t) < 1e9]
        if not later:
            break
        now = max(now + 1e-6, min(later))
    wait_for(msgs)
    if log is not None:
        log.append((now, max(arrival.values()), max(v for k, v in arrival.items() if k[0] == 0)))
    return msgs, steps


def kernel(
    msgs, steps, index,
    tok_hbm, gain_hbm, upw_hbm, upsc_hbm, dnw_hbm, dnsc_hbm, out_ref,
    tok, gain_ref, upw_ref, upsc_ref, dnw_ref, dnsc_ref,
    up_buf, dn_buf, acc, hid, psend, precv, pown, sbuf, r1, r2, fbuf, gbuf, out_t,
    in_sem, w_send, w_recv, d_send, d_recv, s_send, s_recv, f_send, f_recv, x_send, x_recv,
):
    fs, tp = lax.axis_index("fs"), lax.axis_index("tp")
    z, y = lax.div(fs, R), lax.rem(fs, R)
    x, c = lax.div(tp, 2), lax.rem(tp, 2)

    def near(axis, g):
        if axis == "y":
            return (z * R + lax.rem(y + (g + R), R), tp)
        if axis == "z":
            return (lax.rem(z + (g + R), R) * R + y, tp)
        return (fs, lax.rem(x + (g + 4), 4) * 2 + c)

    links = {(a, g): near(a, g) for a in "yz" for g in (1, -1)}
    right, left = near("x", 1), near("x", -1)
    partner = (fs, x * 2 + 1 - c)
    across = [(fs, lax.rem(x + g, 4) * 2 + 1 - c) for g in (1, 3)]

    barrier = pltpu.get_barrier_semaphore()
    peers = list(links.values()) + [right, left, partner] + across
    for peer in peers:
        pl.semaphore_signal(barrier, inc=1, device_id=peer, device_id_type=MESH)

    pairs = (
        (upw_hbm, upw_ref), (dnw_hbm, dnw_ref), (tok_hbm, tok),
        (gain_hbm, gain_ref), (upsc_hbm, upsc_ref), (dnsc_hbm, dnsc_ref),
    )
    loads = [pltpu.make_async_copy(a, b, in_sem.at[n]) for n, (a, b) in enumerate(pairs)]
    for load in loads:
        load.start()

    bufs = (up_buf, dn_buf)
    ys = {d: lax.rem(y + (d + R), R) for d in range(-4, 5)}
    zs = {d: lax.rem(z + (d + R), R) for d in range(-4, 5)}

    def shard_row(dy, dz):
        return zs[dz] * 256 + ys[dy] * 32

    mine = pl.multiple_of(shard_row(0, 0), 32)
    loads[0].wait()
    up_buf[pl.ds(mine, 32), :] = upw_ref[...].astype(jnp.bfloat16)
    loads[1].wait()
    dn_buf[pl.ds(mine, 32), :] = dnw_ref[...].astype(jnp.bfloat16)

    pl.semaphore_wait(barrier, len(peers))

    def copy_of(k, sending):
        axis, g = msgs[k][0]
        dy, dz = offset_yz(k)
        if sending:
            dy, dz = (dy + g, dz) if axis == "y" else (dy, dz + g)
        row = pl.multiple_of(shard_row(dy, dz) + k[1] * ROWS, ROWS)
        ref = bufs[k[0]].at[pl.ds(row, ROWS), :]
        return pltpu.make_async_remote_copy(
            src_ref=ref, dst_ref=ref,
            send_sem=w_send.at[k[0] * 2 + k[1]], recv_sem=w_recv.at[index[k]],
            device_id=links[(axis, g)], device_id_type=MESH,
        )

    def norm(i):
        if i == 0:
            for load in loads[2:]:
                load.wait()
        rows = pl.ds(i * 128, 128)
        v = tok[rows, :].astype(jnp.float32)
        scale = lax.rsqrt(jnp.mean(v * v, axis=-1, keepdims=True) + 1e-6)
        tok[rows, :] = (v * scale * gain_ref[...]).astype(jnp.bfloat16)

    seen = [0] * 4

    def up(j):
        i, n = j // 4, j % 4
        cols = pl.ds(n * 256, 256)
        depth = pl.ds(pl.multiple_of(zs[COLS[i]] * 256, 256), 256)
        pre = jnp.dot(tok[:, depth], up_buf[depth, cols], preferred_element_type=jnp.float32)
        if seen[n] > 0:
            pre = acc[:, cols] + pre
        if seen[n] < 7:
            acc[:, cols] = pre
        else:
            pre = jnp.maximum(pre * upsc_ref[:, cols], 0.0)
            hid[cols, :] = (pre * pre).T.astype(jnp.bfloat16)
        seen[n] += 1

    def pair_copy(i):
        return pltpu.make_async_remote_copy(
            src_ref=psend.at[i], dst_ref=precv.at[i], send_sem=d_send, recv_sem=d_recv.at[i],
            device_id=partner, device_id_type=MESH,
        )

    def relay_copy(i, side):
        return pltpu.make_async_remote_copy(
            src_ref=sbuf.at[i, side], dst_ref=r1.at[i, side], send_sem=s_send, recv_sem=s_recv.at[i, side],
            device_id=(right, left)[side], device_id_type=MESH,
        )

    def final_copy(i, side):
        return pltpu.make_async_remote_copy(
            src_ref=fbuf.at[i, side], dst_ref=gbuf.at[i, side], send_sem=f_send, recv_sem=f_recv.at[i, side],
            device_id=(right, left)[side], device_id_type=MESH,
        )

    def row_in_block(i):
        return ys[COLS[i // 2]] * 32 + (i % 2) * ROWS

    def step_d(i):
        rows = [row_in_block(i) + parity * 256 + k * 512 for parity in (1 - c, c) for k in range(4)]
        lhs = jnp.concatenate([dn_buf[pl.ds(pl.multiple_of(r, ROWS), ROWS), :] for r in rows], axis=0)
        part = jnp.dot(lhs, hid[...], preferred_element_type=jnp.float32)
        psend[i] = part[:64].reshape(4, ROWS, 768).astype(jnp.bfloat16)
        pown[i] = part[64:].reshape(4, ROWS, 768)
        pair_copy(i).start()

    def summed(i, k):
        return pown[i, k] + precv[i, k].astype(jnp.float32)

    def step_e(i):
        pair_copy(i).wait_recv()
        k_far, k_right, k_left = lax.rem(x + 2, 4), lax.rem(x + 1, 4), lax.rem(x + 3, 4)
        total = summed(i, k_far).astype(jnp.bfloat16)
        sbuf[i, 0] = total[:, :384]
        sbuf[i, 1] = total[:, 384:]
        for k in (k_right, k_left):
            pown[i, k] = summed(i, k)
        relay_copy(i, 0).start()
        relay_copy(i, 1).start()
        pown[i, x] = summed(i, x)

    def step_f(i):
        for side in (0, 1):
            relay_copy(i, side).wait_recv()
            own = pown[i, lax.rem(x + (1, 3)[side], 4)]
            extra = r1[i, side].astype(jnp.float32)
            head, tail = own[:, :384], own[:, 384:]
            if side == 0:
                head = head + extra
            else:
                tail = tail + extra
            fbuf[i, side, :, :384] = head.astype(jnp.bfloat16)
            fbuf[i, side, :, 384:] = tail.astype(jnp.bfloat16)
            final_copy(i, side).start()

    late = [arg for name, arg in steps if name == "L"]

    def across_copy(i, side):
        return pltpu.make_async_remote_copy(
            src_ref=psend.at[i, lax.rem(x + 2, 4), :, pl.ds(side * 384, 384)], dst_ref=r2.at[late.index(i), side],
            send_sem=x_send, recv_sem=x_recv.at[late.index(i), side],
            device_id=across[side], device_id_type=MESH,
        )

    def step_l(i):
        step_d(i)
        total = pown[i, lax.rem(x + 2, 4)].astype(jnp.bfloat16)
        sbuf[i, 0] = total[:, :384]
        sbuf[i, 1] = total[:, 384:]
        for side in (0, 1):
            across_copy(i, side).start()
            relay_copy(i, side).start()

    def step_m(i):
        pair_copy(i).wait_recv()
        for side in (0, 1):
            relay_copy(i, side).wait_recv()
            across_copy(i, side).wait_recv()
            own = summed(i, lax.rem(x + (1, 3)[side], 4))
            extra = r1[i, side].astype(jnp.float32) + r2[late.index(i), side].astype(jnp.float32)
            head, tail = own[:, :384], own[:, 384:]
            if side == 0:
                head = head + extra
            else:
                tail = tail + extra
            fbuf[i, side, :, :384] = head.astype(jnp.bfloat16)
            fbuf[i, side, :, 384:] = tail.astype(jnp.bfloat16)
            final_copy(i, side).start()
        pown[i, x] = summed(i, x)

    def step_g(i):
        total = pown[i, x]
        for side in (0, 1):
            final_copy(i, side).wait_recv()
            total = total + gbuf[i, side].astype(jnp.float32)
        out_t[pl.ds(pl.multiple_of(row_in_block(i), ROWS), ROWS), :] = total

    run = {"norm": norm, "U": up, "D": step_d, "E": step_e, "F": step_f, "G": step_g, "L": step_l, "M": step_m}
    for name, arg in steps:
        if name == "wait":
            copy_of(arg, False).wait_recv()
        elif name == "send":
            copy_of(arg, True).start()
        else:
            run[name](arg)

    scale = dnsc_ref[:, pl.ds(pl.multiple_of(tp * 256, 256), 256)]
    out_ref[...] = (out_t[...].T * scale).astype(jnp.bfloat16)

    def sent(ref, sem):
        pltpu.make_async_copy(ref, ref, sem).wait()

    for t in (0, 1):
        for h in (0, 1):
            sent(bufs[t].at[pl.ds(0, 63 * ROWS), :], w_send.at[t * 2 + h])
    sent(psend, d_send)
    sent(sbuf, s_send)
    sent(fbuf, f_send)
    sent(r2, x_send)


def scoped_kernel(msgs, steps, index, *refs):
    dma = pltpu.SemaphoreType.DMA
    pl.run_scoped(
        functools.partial(kernel, msgs, steps, index, *refs),
        dma((6,)), dma((4,)), dma((len(msgs),)), dma, dma((16,)),
        dma, dma((16, 2)), dma, dma((16, 2)), dma, dma((LAST, 2)),
    )


def on_device(tokens, norm_gain, up_weight, up_scale, down_weight, down_scale):
    msgs, steps = plan()
    index = {k: i for i, k in enumerate(msgs)}
    bf16, f32 = jnp.bfloat16, jnp.float32
    return pl.pallas_call(
        functools.partial(scoped_kernel, msgs, steps, index),
        out_shape=pltpu.VMEM((768, 256), bf16),
        in_specs=[pl.BlockSpec(memory_space=pl.ANY)] * 6,
        out_specs=pl.BlockSpec(memory_space=pltpu.VMEM),
        scratch_shapes=[
            pltpu.VMEM((768, 2048), bf16),
            pltpu.VMEM((1, 2048), f32),
            pltpu.VMEM((32, 1024), f32),
            pltpu.VMEM((1, 1024), f32),
            pltpu.VMEM((32, 1024), f32),
            pltpu.VMEM((1, 2048), f32),
            pltpu.VMEM((2048, 1024), bf16),
            pltpu.VMEM((2048, 1024), bf16),
            pltpu.VMEM((768, 1024), f32),
            pltpu.VMEM((1024, 768), bf16),
            pltpu.VMEM((16, 4, 16, 768), bf16),
            pltpu.VMEM((16, 4, 16, 768), bf16),
            pltpu.VMEM((16, 4, 16, 768), f32),
            pltpu.VMEM((16, 2, 16, 384), bf16),
            pltpu.VMEM((16, 2, 16, 384), bf16),
            pltpu.VMEM((LAST, 2, 16, 384), bf16),
            pltpu.VMEM((16, 2, 16, 768), bf16),
            pltpu.VMEM((16, 2, 16, 768), bf16),
            pltpu.VMEM((256, 768), f32),
        ],
        compiler_params=pltpu.CompilerParams(collective_id=0, has_side_effects=True),
    )(
        tokens, norm_gain.reshape(1, -1), up_weight, up_scale.reshape(1, -1), down_weight.T,
        down_scale,
    )


def solution(mesh):
    in_specs = (P("fs", None), P(), P("fs", "tp"), P("tp"), P("tp", "fs"), P())
    return jax.shard_map(
        on_device, mesh=mesh, in_specs=in_specs, out_specs=P("fs", "tp"), check_vma=False
    )
```
